32 devices in a mesh: sp: 8 (over z, y), tp: 4 (over x, core).
Axes of the slice: x: 2, y: 2, z: 4, core: 2. Of those that a mesh axis runs over, the one named last changes fastest.
Arguments:
- queries: bfloat16 [2048, 2048], P('sp', 'tp'), may hold values from -9 to 9
- keys: bfloat16 [2048, 1024], P('sp', 'tp'), may hold values from -9 to 9
- values: bfloat16 [2048, 1024], P('sp', 'tp'), may hold values from -6 to 6
- lam: float32 [8], P('tp'), may hold values from 0.3 to 0.8
- diff_gain: float32 [256], replicated, may hold values from 0.1 to 1.9
- lin_query: bfloat16 [2048, 512], P('sp', 'tp'), may hold values from -6 to 6
- lin_key: bfloat16 [2048, 512], P('sp', 'tp'), may hold values from -6 to 6
- lin_value: bfloat16 [2048, 1024], P('sp', 'tp'), may hold values from -6 to 6
- decay_pre: float32 [2048, 512], P('sp', 'tp'), may hold values from -14 to 14
- lin_gain: float32 [1024], P('tp'), may hold values from 0.1 to 1.9
- w_out_diff: bfloat16 [2048, 4096], P('tp'), may hold values from -0.125 to 0.125
- w_out_lin: bfloat16 [1024, 4096], P('tp'), may hold values from -0.1875 to 0.1875
Outputs:
- mixed: bfloat16 [2048, 4096], P(('sp', 'tp'))
The draws below stay inside these ranges and needn't reach their ends.
All inputs are finite; a program needn't handle non-finite values.
Results may differ from the reference program's by a relative error of at most 0.015.
Values may be sent and summed in bfloat16 or wider, within the bound.
A program may use at most 128 MiB of HBM per device.

```python
import math
import jax
import jax.numpy as jnp
from jax import lax

D = 4096
DIFF_HEADS = 8
KV_HEADS = 4
LIN_HEADS = 4
HEAD_DIM = 128
KEY_DIM = 128
VAL_DIM = 256
BLOCK = 64
TOK_DEV = 256
SEQUENCE_TOKENS = 2048
N_TP = 4


gate_temp = 16.0


def paired_draw(key):
    query_key = jax.random.fold_in(key, 101)
    key_key = jax.random.fold_in(key, 102)
    query_shape = (SEQUENCE_TOKENS, DIFF_HEADS * 2 * HEAD_DIM)
    key_shape = (SEQUENCE_TOKENS, KV_HEADS * 2 * HEAD_DIM)
    spread = 1.32
    query_rows = jnp.clip(spread * jax.random.normal(query_key, query_shape, jnp.float32), -5.0, 5.0)
    key_rows = jnp.clip(spread * jax.random.normal(key_key, key_shape, jnp.float32), -5.0, 5.0)
    return (query_rows, key_rows)


def draw_queries(key, part):
    return paired_draw(key)[0].astype(jnp.bfloat16)


def draw_keys(key, part):
    return paired_draw(key)[1].astype(jnp.bfloat16)


def draw_decay_pre(key, part):
    width = LIN_HEADS * KEY_DIM
    random_subkeys = jax.random.split(jax.random.fold_in(key, 201), 8)
    fast_share = 0.5
    is_fast = jax.random.uniform(random_subkeys[0], (width,), jnp.float32) < fast_share
    fast_rate = jnp.exp(jax.random.uniform(random_subkeys[1], (width,), jnp.float32, math.log(0.01), math.log(1.0 / 30.0)))
    slow_rate = jnp.exp(jax.random.uniform(random_subkeys[2], (width,), jnp.float32, math.log(0.05), math.log(0.25))) / SEQUENCE_TOKENS
    decay_speed = jnp.where(is_fast, fast_rate, slow_rate)
    processor_factor = jnp.exp(jax.random.uniform(random_subkeys[3], (SEQUENCE_TOKENS // TOK_DEV,), jnp.float32, math.log(0.5), math.log(2.0)))
    processor_factor = jnp.repeat(processor_factor, TOK_DEV)[:, None]
    jaggedness = jax.random.uniform(random_subkeys[4], (SEQUENCE_TOKENS, width), jnp.float32, 0.5, 1.5)
    spike_position = jax.random.randint(random_subkeys[5], (3,), 0, SEQUENCE_TOKENS, dtype=jnp.int32)
    spike_length = jax.random.uniform(random_subkeys[6], (3,), jnp.float32, 0.22, 0.6)
    token_positions = jnp.arange(SEQUENCE_TOKENS, dtype=jnp.int32)
    spike_rows = jnp.sum(jnp.where(token_positions[:, None] == spike_position[None, :], spike_length[None, :], 0.0), axis=1)[:, None]
    logarithm_decay = -(decay_speed[None, :] * processor_factor * jaggedness) - spike_rows
    scaled = gate_temp * logarithm_decay
    return -jnp.log(jnp.expm1(-scaled))


def steps_of(stream_key, dims, cuts, low, high):
    loudness, own = 1.0, jax.random.fold_in(stream_key, 6)
    for position, parts in cuts:
        draws = jnp.exp(jax.random.uniform(jax.random.fold_in(own, position), (parts,), jnp.float32, low / len(cuts), high / len(cuts)))
        loudness = loudness * jnp.repeat(draws, dims[position] // parts).reshape([-1 if axis == position else 1 for axis in range(len(dims))])
    return loudness


def gaussian(stream_key, shape, scale, most, pieces=(), kind=jnp.bfloat16):
    drawn = scale * jax.random.normal(stream_key, shape, jnp.float32)
    if pieces:
        drawn = drawn * steps_of(stream_key, shape, pieces, -0.22, 0.18)
    return jnp.clip(drawn, -most, most).astype(kind)


def setup_inputs(seed: int = 0) -> dict:
    key_of = jax.random.split(jax.random.key(seed), 13)
    queries = draw_queries(jax.random.fold_in(key_of[12], 71), 0)
    keys = draw_keys(jax.random.fold_in(key_of[12], 71), 0)
    values = gaussian(key_of[2], (SEQUENCE_TOKENS, KV_HEADS * VAL_DIM), 1.0, 6.0, ((0, 8), (1, 4)))
    lam = jnp.clip(0.3 + 0.5 * jax.random.uniform(key_of[3], (DIFF_HEADS,), jnp.float32) ** steps_of(key_of[3], (DIFF_HEADS,), ((0, 4),), -0.2, 0.2), 0.3, 0.8)
    diff_gain = jnp.clip(1.0 + 0.18 * jax.random.normal(key_of[4], (VAL_DIM,), jnp.float32), 0.1, 1.9)
    lin_query = gaussian(key_of[5], (SEQUENCE_TOKENS, LIN_HEADS * KEY_DIM), 1.0, 6.0, ((0, 8), (1, 4)))
    lin_key = gaussian(key_of[6], (SEQUENCE_TOKENS, LIN_HEADS * KEY_DIM), 1.0, 6.0, ((0, 8), (1, 4)))
    lin_value = gaussian(key_of[7], (SEQUENCE_TOKENS, LIN_HEADS * VAL_DIM), 1.0, 6.0, ((0, 8), (1, 4)))
    decay_pre = draw_decay_pre(jax.random.fold_in(key_of[12], 71), 0)
    lin_gain = jnp.clip(1.0 + 0.18 * jax.random.normal(key_of[9], (LIN_HEADS * VAL_DIM,), jnp.float32), 0.1, 1.9)
    w_out_diff = gaussian(key_of[10], (DIFF_HEADS * VAL_DIM, D), (DIFF_HEADS * VAL_DIM) ** -0.5, 0.125, ((0, 4),))
    w_out_lin = gaussian(key_of[11], (LIN_HEADS * VAL_DIM, D), (LIN_HEADS * VAL_DIM) ** -0.5, 0.1875, ((0, 4),))
    return {"queries": queries, "keys": keys, "values": values, "lam": lam, "diff_gain": diff_gain, "lin_query": lin_query, "lin_key": lin_key, "lin_value": lin_value, "decay_pre": decay_pre, "lin_gain": lin_gain, "w_out_diff": w_out_diff, "w_out_lin": w_out_lin}


norm_eps = 1e-06
gate_temp = 16.0
neg_large = -1e+30
highest = lax.Precision.HIGHEST

def head_norm(mixed_in, gain):
    return mixed_in * lax.rsqrt(lax.optimization_barrier(jnp.mean(mixed_in * mixed_in, axis=-1, keepdims=True)) + norm_eps) * gain

def one_map(query_rows, key_rows, value_rows, query_pos, key_pos):
    scores = jnp.einsum('jqd,sd->jqs', query_rows, key_rows) / math.sqrt(HEAD_DIM)
    allowed = query_pos[:, None] >= key_pos[None, :]
    scores = jnp.where(allowed, scores, neg_large)
    row_top = lax.optimization_barrier(jnp.max(scores, axis=-1, keepdims=True))
    expo = jnp.where(allowed, jnp.exp(scores - row_top), 0.0)
    totals = lax.optimization_barrier(jnp.sum(expo, axis=-1))
    weights = lax.optimization_barrier(expo.astype(jnp.bfloat16)).astype(jnp.float32)
    numer = jnp.einsum('jqs,se->jqe', weights, value_rows)
    return numer / totals[..., None]

def diff_attention(queries, keys, values, lam, diff_gain):
    group_size = DIFF_HEADS // KV_HEADS
    query_all = queries.astype(jnp.float32).reshape(SEQUENCE_TOKENS, KV_HEADS, group_size, 2, HEAD_DIM)
    key_all = keys.astype(jnp.float32).reshape(SEQUENCE_TOKENS, KV_HEADS, 2, HEAD_DIM)
    value_all = values.astype(jnp.float32).reshape(SEQUENCE_TOKENS, KV_HEADS, VAL_DIM)
    lam_grid = lam.reshape(KV_HEADS, group_size)
    span_rows = math.gcd(SEQUENCE_TOKENS, 1024)
    outputs = []
    for block_index in range(SEQUENCE_TOKENS // span_rows):
        begin = block_index * span_rows
        limit = begin + span_rows
        query_pos = begin + jnp.arange(span_rows, dtype=jnp.int32)
        key_pos = jnp.arange(limit, dtype=jnp.int32)
        query_rows = query_all[begin:limit].transpose(1, 2, 3, 0, 4)
        key_rows = key_all[:limit].transpose(1, 2, 0, 3)
        value_rows = value_all[:limit].transpose(1, 0, 2)

        def per_group(operands):
            query_group, key_group, value_group, lam_group = operands
            first_out = one_map(query_group[:, 0], key_group[0], value_group, query_pos, key_pos)
            second_out = one_map(query_group[:, 1], key_group[1], value_group, query_pos, key_pos)
            return first_out - lam_group[:, None, None] * second_out
        attended = lax.map(per_group, (query_rows, key_rows, value_rows, lam_grid))
        normed = head_norm(attended, diff_gain).astype(jnp.bfloat16)
        outputs.append(normed.transpose(2, 0, 1, 3).reshape(span_rows, DIFF_HEADS * VAL_DIM))
    return jnp.concatenate(outputs, axis=0)

def gla_step(run_state, inputs):
    query_blk, key_blk, value_blk, decay_blk = inputs
    length = query_blk.shape[1]
    cumulative = jnp.cumsum(decay_blk, axis=1)
    lower_mask = jnp.tril(jnp.ones((length, length), dtype=bool))[None, :, :, None]
    spread = jnp.where(lower_mask, cumulative[:, :, None, :] - cumulative[:, None, :, :], 0.0)
    factor = jnp.where(lower_mask, jnp.exp(spread), 0.0)
    inner = jnp.einsum('htd,hsd,htsd->hts', query_blk, key_blk, factor, precision=highest)
    local_part = jnp.einsum('hts,hse->hte', inner, value_blk, precision=highest)
    carried = jnp.einsum('htd,hde->hte', query_blk * jnp.exp(cumulative), run_state, precision=highest)
    last_sum = cumulative[:, -1:, :]
    new_state = jnp.exp(last_sum[:, 0, :])[..., None] * run_state + jnp.einsum('hsd,hse->hde', key_blk * jnp.exp(last_sum - cumulative), value_blk, precision=highest)
    return (new_state, local_part + carried)

def linear_attention(lin_query, lin_key, lin_value, decay_pre, lin_gain):
    block_count = SEQUENCE_TOKENS // BLOCK

    def arrange(array, width):
        return array.astype(jnp.float32).reshape(block_count, BLOCK, LIN_HEADS, width).transpose(0, 2, 1, 3)
    start_state = jnp.zeros((LIN_HEADS, KEY_DIM, VAL_DIM), jnp.float32)
    _, outputs = lax.scan(gla_step, start_state, (arrange(lin_query, KEY_DIM) * KEY_DIM ** (-0.5), arrange(lin_key, KEY_DIM), arrange(lin_value, VAL_DIM), arrange(jax.nn.log_sigmoid(decay_pre) / gate_temp, KEY_DIM)))
    linear_rows = outputs.transpose(0, 2, 1, 3).reshape(SEQUENCE_TOKENS, LIN_HEADS, VAL_DIM)
    normed = head_norm(linear_rows, lin_gain.reshape(LIN_HEADS, VAL_DIM)).astype(jnp.bfloat16)
    return normed.reshape(SEQUENCE_TOKENS, LIN_HEADS * VAL_DIM)

def reference(queries, keys, values, lam, diff_gain, lin_query, lin_key, lin_value, decay_pre, lin_gain, w_out_diff, w_out_lin):
    diff_out = diff_attention(queries, keys, values, lam, diff_gain)
    lin_out = linear_attention(lin_query, lin_key, lin_value, decay_pre, lin_gain)
    diff_cols = DIFF_HEADS * VAL_DIM // N_TP
    lin_cols = LIN_HEADS * VAL_DIM // N_TP
    summed = jnp.zeros((SEQUENCE_TOKENS, D), jnp.float32)
    for member in range(N_TP):
        diff_lo = member * diff_cols
        lin_lo = member * lin_cols
        partial_value = jnp.dot(diff_out[:, diff_lo:diff_lo + diff_cols], w_out_diff[diff_lo:diff_lo + diff_cols], preferred_element_type=jnp.float32)
        partial_value = partial_value + jnp.dot(lin_out[:, lin_lo:lin_lo + lin_cols], w_out_lin[lin_lo:lin_lo + lin_cols], preferred_element_type=jnp.float32)
        partial_value = lax.optimization_barrier(partial_value.astype(jnp.bfloat16)).astype(jnp.float32)
        summed = summed + partial_value
    return summed.astype(jnp.bfloat16)
```

```python
import functools
import math

import jax
import jax.numpy as jnp
from jax import lax
from jax.experimental import pallas as pl
from jax.experimental.pallas import tpu as pltpu
from jax.sharding import PartitionSpec as P

HEAD_DIM = 128
KEY_DIM = 128
VAL_DIM = 256
BLOCK = 64
PIECE = 512

norm_eps = 1e-06
gate_temp = 16.0
neg_large = -1e30
highest = lax.Precision.HIGHEST
MESH = pl.DeviceIdType.MESH
F32 = jnp.float32
BF16 = jnp.bfloat16


def dot(a, b, dims, precision=None):
    return lax.dot_general(
        a, b, (dims, ((), ())), precision=precision, preferred_element_type=F32
    )


NN = ((1,), (0,))
NT = ((1,), (1,))
TN = ((0,), (0,))


def head_norm(rows, gain):
    return rows * lax.rsqrt(jnp.mean(rows * rows, axis=-1, keepdims=True) + norm_eps) * gain


def kernel(
    n_sp,
    n_tp,
    q_ref,
    k_ref,
    v_ref,
    lam_ref,
    dgain_ref,
    lq_ref,
    lk_ref,
    lv_ref,
    pre_ref,
    lgain_ref,
    wd_ref,
    wl_ref,
    out_ref,
    zk,
    zv,
    yk,
    yv,
    qs,
    top,
    total,
    numer,
    msg,
    got,
    chain_in,
    chain_out,
    own_state,
    reach,
    rows_ref,
    act,
    weights,
    part,
    pair_buf,
    sum_buf,
    own_sum,
    cross_buf,
    w_sem,
    zk_send,
    zk_recv,
    zv_send,
    zv_recv,
    yk_send,
    yk_recv,
    yv_send,
    yv_recv,
    s_send,
    s_recv,
    c_send,
    c_recv,
    p_send,
    p_recv,
    x_send,
    x_recv,
):
    outer_n = n_sp // 2
    half = n_tp // 2
    tok = q_ref.shape[0]
    kv_here = k_ref.shape[1] // (2 * HEAD_DIM)
    heads = q_ref.shape[1] // (2 * HEAD_DIM)
    group = heads // kv_here
    lin_heads = lq_ref.shape[1] // KEY_DIM
    diff_rows = wd_ref.shape[0]
    me = lax.axis_index("sp")
    tp = lax.axis_index("tp")
    outer = me // 2
    inner = lax.rem(me, 2)
    mate = outer * 2 + (1 - inner)
    ahead = me + 2
    behind = me - 2
    tp_x = tp // 2
    tp_c = lax.rem(tp, 2)
    tp_mate = tp_x * 2 + (1 - tp_c)
    has_next = outer < outer_n - 1
    has_prev = outer > 0

    w_copies = (
        pltpu.make_async_copy(wd_ref, weights.at[pl.ds(0, diff_rows)], w_sem.at[0]),
        pltpu.make_async_copy(
            wl_ref, weights.at[pl.ds(diff_rows, wl_ref.shape[0])], w_sem.at[1]
        ),
    )
    for copy in w_copies:
        copy.start()

    barrier = pltpu.get_barrier_semaphore()

    def greet(where):
        pl.semaphore_signal(barrier, inc=1, device_id=where, device_id_type=MESH)

    greet({"sp": mate})
    greet({"tp": tp_mate})
    for step in range(1, half):
        greet({"tp": lax.rem(tp_x + step, half) * 2 + tp_c})

    @pl.when(has_next)
    def _():
        greet({"sp": ahead})

    @pl.when(has_prev)
    def _():
        greet({"sp": behind})

    pl.semaphore_wait(
        barrier, 1 + half + has_next.astype(jnp.int32) + has_prev.astype(jnp.int32)
    )

    def remote(src, dst, send, recv, where):
        return pltpu.make_async_remote_copy(
            src_ref=src,
            dst_ref=dst,
            send_sem=send,
            recv_sem=recv,
            device_id=where,
            device_id_type=MESH,
        )

    def z_k(s, src):
        return remote(src, zk.at[s + 1], zk_send.at[s], zk_recv.at[s + 1], {"sp": ahead})

    def z_v(s, src):
        return remote(src, zv.at[s + 1], zv_send.at[s], zv_recv.at[s + 1], {"sp": ahead})

    def y_k(s, src):
        return remote(src, yk.at[s], yk_send.at[s], yk_recv.at[s], {"sp": mate})

    def y_v(s, src):
        return remote(src, yv.at[s], yv_send.at[s], yv_recv.at[s], {"sp": mate})

    @pl.when(has_next)
    def _():
        z_k(0, k_ref).start()

    @pl.when(inner == 0)
    def _():
        y_k(0, k_ref).start()

    @pl.when(has_next)
    def _():
        z_v(0, v_ref).start()

    length = math.gcd(tok, BLOCK)
    low = lax.broadcasted_iota(jnp.int32, (length, length), 0) >= lax.broadcasted_iota(
        jnp.int32, (length, length), 1
    )
    tri = low.astype(F32)
    for h in range(lin_heads):
        kc = pl.ds(h * KEY_DIM, KEY_DIM)
        vc = pl.ds(h * VAL_DIM, VAL_DIM)
        state = None
        passed = jnp.zeros((1, KEY_DIM), F32)
        for b in range(tok // length):
            r = pl.ds(b * length, length)
            pre = pre_ref[r, kc]
            log_decay = (jnp.minimum(pre, 0.0) - jnp.log1p(jnp.exp(-jnp.abs(pre)))) / gate_temp
            cumulative = dot(tri, log_decay, NN, highest)
            last = cumulative[length - 1 :, :]
            query = lq_ref[r, kc].astype(F32) * (KEY_DIM**-0.5) * jnp.exp(cumulative)
            key = lk_ref[r, kc].astype(F32)
            value = lv_ref[r, vc].astype(F32)
            inside = dot(query, key * jnp.exp(-cumulative), NT, highest)
            inside = jnp.where(low, inside, 0.0)
            rows = dot(inside, value, NN, highest)
            fresh = dot(value, key * jnp.exp(last - cumulative), TN, highest)
            if state is not None:
                rows = rows + dot(query, state, NT, highest)
                fresh = fresh + jnp.exp(last) * state
            rows_ref[r, vc] = rows
            reach[r, kc] = query * jnp.exp(passed)
            state = fresh
            passed = passed + last
        own_state[h, pl.ds(0, VAL_DIM), :] = state
        own_state[h, pl.ds(VAL_DIM, 8), :] = jnp.broadcast_to(passed, (8, KEY_DIM))
        msg[h, pl.ds(0, VAL_DIM), :] = state.astype(BF16)
        high = passed.astype(BF16).astype(F32)
        pick = lax.broadcasted_iota(jnp.int32, (16, KEY_DIM), 0) < 8
        msg[h, pl.ds(VAL_DIM, 16), :] = jnp.where(pick, high, passed - high).astype(BF16)

    s_copy = remote(msg, got, s_send, s_recv, {"sp": mate})
    s_copy.start()

    @pl.when(inner == 0)
    def _():
        y_v(0, v_ref).start()

    for g in range(kv_here):
        for m in range(2):
            for j in range(group):
                col = ((g * group + j) * 2 + m) * HEAD_DIM
                qs[g, m, pl.ds(j * tok, tok), :] = q_ref[:, pl.ds(col, HEAD_DIM)]

    rate = math.log2(math.e) / math.sqrt(HEAD_DIM)
    stacked = group * tok

    def attend(key_ref, value_ref, first):
        for g in range(kv_here):
            value = value_ref[:, pl.ds(g * VAL_DIM, VAL_DIM)]
            for m in range(2):
                key = key_ref[:, pl.ds((g * 2 + m) * HEAD_DIM, HEAD_DIM)]
                scores = dot(qs[g, m], key, NT)
                if first:
                    at_row = lax.rem(lax.broadcasted_iota(jnp.int32, (stacked, tok), 0), tok)
                    at_col = lax.broadcasted_iota(jnp.int32, (stacked, tok), 1)
                    scores = jnp.where(at_row >= at_col, scores, neg_large)
                best = jnp.max(scores, axis=-1, keepdims=True)
                if not first:
                    old = top[g, m]
                    best = jnp.maximum(old, best)
                expo = jnp.exp2((scores - best) * rate)
                add = jnp.sum(expo, axis=-1, keepdims=True)
                grown = dot(expo.astype(BF16), value, NN)
                if first:
                    total[g, m] = add
                    numer[g, m] = grown
                else:
                    shrink = jnp.exp2((old - best) * rate)
                    total[g, m] = total[g, m] * shrink + add
                    numer[g, m] = numer[g, m] * shrink + grown
                top[g, m] = best

    attend(k_ref, v_ref, True)

    def from_mate(t):
        y_k(t, yk.at[t]).wait_recv()
        y_v(t, yv.at[t]).wait_recv()
        attend(yk.at[t], yv.at[t], False)

    def hop(s, carry):
        remote(zk.at[s], zk.at[s], zk_send.at[s], zk_recv.at[s], {"sp": mate}).wait_recv()

        @pl.when(has_next)
        def _():
            z_k(s, zk.at[s]).start()

        y_k(s, zk.at[s]).start()
        remote(zv.at[s], zv.at[s], zv_send.at[s], zv_recv.at[s], {"sp": mate}).wait_recv()

        @pl.when(has_next)
        def _():
            z_v(s, zv.at[s]).start()

        y_v(s, zv.at[s]).start()
        attend(zk.at[s], zv.at[s], False)

        @pl.when((s > 1) | (inner == 1))
        def _():
            from_mate(s - 1)

        return carry

    lax.fori_loop(1, outer + 1, hop, 0)

    s_copy.wait_recv()
    c_copy = remote(chain_out, chain_in, c_send, c_recv, {"sp": ahead})

    @pl.when(has_prev)
    def _():
        c_copy.wait_recv()

    @pl.when(jnp.logical_not(has_prev))
    def _():
        chain_in[...] = jnp.zeros_like(chain_in)

    for h in range(lin_heads):
        mine = own_state[h, pl.ds(0, VAL_DIM), :]
        mine_decay = own_state[h, pl.ds(VAL_DIM, 8), :][:1]
        theirs = got[h, pl.ds(0, VAL_DIM), :].astype(F32)
        tail = got[h, pl.ds(VAL_DIM, 16), :].astype(F32)
        theirs_decay = tail[:1] + tail[8:9]
        before = chain_in[h].astype(F32)
        to_first = jnp.exp(theirs_decay) * before + theirs
        incoming = jnp.where(inner == 1, to_first, before)
        both = jnp.exp(mine_decay) * to_first + mine
        other = jnp.exp(theirs_decay) * (jnp.exp(mine_decay) * before + mine) + theirs
        chain_out[h] = jnp.where(inner == 1, both, other).astype(BF16)
        own_state[h, pl.ds(0, VAL_DIM), :] = incoming

    @pl.when(has_next)
    def _():
        c_copy.start()

    for h in range(lin_heads):
        kc = pl.ds(h * KEY_DIM, KEY_DIM)
        vc = pl.ds(h * VAL_DIM, VAL_DIM)
        rows = rows_ref[:, vc] + dot(
            reach[:, kc], own_state[h, pl.ds(0, VAL_DIM), :], NT, highest
        )
        act[:, pl.ds(diff_rows + h * VAL_DIM, VAL_DIM)] = head_norm(
            rows, lgain_ref[:, vc]
        ).astype(BF16)

    @pl.when(has_prev | (inner == 1))
    def _():
        from_mate(outer)

    for g in range(kv_here):
        for j in range(group):
            h = g * group + j
            r = pl.ds(j * tok, tok)
            attended = numer[g, 0, r, :] / total[g, 0, r, :] - lam_ref[h] * (
                numer[g, 1, r, :] / total[g, 1, r, :]
            )
            act[:, pl.ds(h * VAL_DIM, VAL_DIM)] = head_norm(attended, dgain_ref[...]).astype(BF16)

    for copy in w_copies:
        copy.wait()

    width = part.shape[-1]
    pieces = part.shape[0]
    rows_each = tok // n_tp

    def pair_copy(j):
        return remote(
            part.at[j, 1 - tp_c], pair_buf.at[j], p_send.at[j], p_recv.at[j], {"tp": tp_mate}
        )

    def cross_copy(j, step):
        to = lax.rem(tp_x + step, half)
        return remote(
            sum_buf.at[j, step - 1],
            cross_buf.at[j, step - 1],
            x_send.at[j, step - 1],
            x_recv.at[j, step - 1],
            {"tp": to * 2 + tp_c},
        )

    def reduce_pair(j):
        pair_copy(j).wait_recv()
        for step in range(1, half):
            to = lax.rem(tp_x + step, half)
            sum_buf[j, step - 1] = (
                part[j, tp_c, to].astype(F32) + pair_buf[j, to].astype(F32)
            ).astype(BF16)
            cross_copy(j, step).start()
        own_sum[j] = part[j, tp_c, tp_x].astype(F32) + pair_buf[j, tp_x].astype(F32)

    def project(j, carry):
        cols = pl.ds(pl.multiple_of(j * width, width), width)
        piece = dot(act[...], weights[:, cols], NN).astype(BF16)
        for a in range(half):
            for c in range(2):
                part[j, c, a] = piece[(a * 2 + c) * rows_each : (a * 2 + c + 1) * rows_each]
        pair_copy(j).start()

        @pl.when(j > 0)
        def _():
            reduce_pair(j - 1)

        return carry

    lax.fori_loop(0, pieces, project, 0)
    reduce_pair(pieces - 1)

    def finish(j, carry):
        cols = pl.ds(pl.multiple_of(j * width, width), width)
        whole = own_sum[j]
        for step in range(1, half):
            cross_copy(j, step).wait_recv()
            whole = whole + cross_buf[j, step - 1].astype(F32)
        out_ref[:, cols] = whole.astype(BF16)
        pair_copy(j).wait_send()
        for step in range(1, half):
            cross_copy(j, step).wait_send()
        return carry

    lax.fori_loop(0, pieces, finish, 0)

    s_copy.wait_send()

    @pl.when(inner == 0)
    def _():
        y_k(0, k_ref).wait_send()
        y_v(0, v_ref).wait_send()

    @pl.when(has_next)
    def _():
        z_k(0, k_ref).wait_send()
        z_v(0, v_ref).wait_send()
        c_copy.wait_send()

    def drain(s, carry):
        y_k(s, zk.at[s]).wait_send()
        y_v(s, zv.at[s]).wait_send()

        @pl.when(has_next)
        def _():
            z_k(s, zk.at[s]).wait_send()
            z_v(s, zv.at[s]).wait_send()

        return carry

    lax.fori_loop(1, outer + 1, drain, 0)


def body(
    n_sp,
    n_tp,
    queries,
    keys,
    values,
    lam,
    diff_gain,
    lin_query,
    lin_key,
    lin_value,
    decay_pre,
    lin_gain,
    w_out_diff,
    w_out_lin,
):
    tok = queries.shape[0]
    kv_here = keys.shape[1] // (2 * HEAD_DIM)
    heads = queries.shape[1] // (2 * HEAD_DIM)
    lin_heads = lin_query.shape[1] // KEY_DIM
    model = w_out_diff.shape[1]
    in_rows = w_out_diff.shape[0] + w_out_lin.shape[0]
    stacked = heads // kv_here * tok
    width = math.gcd(model, PIECE)
    pieces = model // width
    half = n_tp // 2
    outer_n = n_sp // 2
    rows_each = tok // n_tp
    vmem = pl.BlockSpec(memory_space=pltpu.VMEM)
    anywhere = pl.BlockSpec(memory_space=pl.ANY)
    smem = pl.BlockSpec(memory_space=pltpu.SMEM)
    dma = pltpu.SemaphoreType.DMA
    return pl.pallas_call(
        functools.partial(kernel, n_sp, n_tp),
        out_shape=jax.ShapeDtypeStruct((rows_each, model), BF16),
        in_specs=[vmem] * 3 + [smem] + [vmem] * 6 + [anywhere] * 2,
        out_specs=vmem,
        scratch_shapes=[
            pltpu.VMEM((outer_n, *keys.shape), BF16),
            pltpu.VMEM((outer_n, *values.shape), BF16),
            pltpu.VMEM((outer_n, *keys.shape), BF16),
            pltpu.VMEM((outer_n, *values.shape), BF16),
            pltpu.VMEM((kv_here, 2, stacked, HEAD_DIM), BF16),
            pltpu.VMEM((kv_here, 2, stacked, 1), F32),
            pltpu.VMEM((kv_here, 2, stacked, 1), F32),
            pltpu.VMEM((kv_here, 2, stacked, VAL_DIM), F32),
            pltpu.VMEM((lin_heads, VAL_DIM + 16, KEY_DIM), BF16),
            pltpu.VMEM((lin_heads, VAL_DIM + 16, KEY_DIM), BF16),
            pltpu.VMEM((lin_heads, VAL_DIM, KEY_DIM), BF16),
            pltpu.VMEM((lin_heads, VAL_DIM, KEY_DIM), BF16),
            pltpu.VMEM((lin_heads, VAL_DIM + 8, KEY_DIM), F32),
            pltpu.VMEM(lin_query.shape, F32),
            pltpu.VMEM(lin_value.shape, F32),
            pltpu.VMEM((tok, in_rows), BF16),
            pltpu.VMEM((in_rows, model), BF16),
            pltpu.VMEM((pieces, 2, half, rows_each, width), BF16),
            pltpu.VMEM((pieces, half, rows_each, width), BF16),
            pltpu.VMEM((pieces, half - 1, rows_each, width), BF16),
            pltpu.VMEM((pieces, rows_each, width), F32),
            pltpu.VMEM((pieces, half - 1, rows_each, width), BF16),
            dma((2,)),
        ]
        + [dma((outer_n,))] * 8
        + [dma] * 4
        + [dma((pieces,))] * 2
        + [dma((pieces, half - 1))] * 2,
        compiler_params=pltpu.CompilerParams(
            collective_id=0, has_side_effects=True, vmem_limit_bytes=60 * 1024 * 1024
        ),
    )(
        queries,
        keys,
        values,
        lam,
        diff_gain.reshape(1, -1),
        lin_query,
        lin_key,
        lin_value,
        decay_pre,
        lin_gain.reshape(1, -1),
        w_out_diff,
        w_out_lin,
    )


def solution(mesh):
    return jax.shard_map(
        functools.partial(body, mesh.shape["sp"], mesh.shape["tp"]),
        mesh=mesh,
        in_specs=(
            P("sp", "tp"),
            P("sp", "tp"),
            P("sp", "tp"),
            P("tp"),
            P(),
            P("sp", "tp"),
            P("sp", "tp"),
            P("sp", "tp"),
            P("sp", "tp"),
            P("tp"),
            P("tp", None),
            P("tp", None),
        ),
        out_specs=P(("sp", "tp"), None),
        check_vma=False,
    )
```

```python
import functools
import math

import jax
import jax.numpy as jnp
from jax import lax
from jax.experimental import pallas as pl
from jax.experimental.pallas import tpu as pltpu
from jax.sharding import PartitionSpec as P

HEAD_DIM = 128
KEY_DIM = 128
VAL_DIM = 256
BLOCK = 64
PIECE = 512

norm_eps = 1e-06
gate_temp = 16.0
neg_large = -1e30
highest = lax.Precision.HIGHEST
MESH = pl.DeviceIdType.MESH
F32 = jnp.float32
BF16 = jnp.bfloat16


def dot(a, b, dims, precision=None):
    return lax.dot_general(
        a, b, (dims, ((), ())), precision=precision, preferred_element_type=F32
    )


NN = ((1,), (0,))
NT = ((1,), (1,))
TN = ((0,), (0,))


def head_norm(rows, gain):
    return rows * lax.rsqrt(jnp.mean(rows * rows, axis=-1, keepdims=True) + norm_eps) * gain


def kernel(
    n_sp,
    n_tp,
    q_ref,
    k_ref,
    v_ref,
    lam_ref,
    dgain_ref,
    lq_ref,
    lk_ref,
    lv_ref,
    pre_ref,
    lgain_ref,
    wd_ref,
    wl_ref,
    out_ref,
    zk,
    zv,
    yk,
    yv,
    qs,
    top,
    total,
    numer,
    msg,
    got,
    chain_in,
    chain_out,
    own_state,
    reach,
    rows_ref,
    act,
    weights,
    part,
    pair_buf,
    sum_buf,
    own_sum,
    cross_buf,
    w_sem,
    zk_send,
    zk_recv,
    zv_send,
    zv_recv,
    yk_send,
    yk_recv,
    yv_send,
    yv_recv,
    s_send,
    s_recv,
    c_send,
    c_recv,
    p_send,
    p_recv,
    x_send,
    x_recv,
):
    outer_n = n_sp // 2
    half = n_tp // 2
    tok = q_ref.shape[0]
    kv_here = k_ref.shape[1] // (2 * HEAD_DIM)
    heads = q_ref.shape[1] // (2 * HEAD_DIM)
    group = heads // kv_here
    lin_heads = lq_ref.shape[1] // KEY_DIM
    diff_rows = wd_ref.shape[0]
    me = lax.axis_index("sp")
    tp = lax.axis_index("tp")
    outer = me // 2
    inner = lax.rem(me, 2)
    mate = outer * 2 + (1 - inner)
    ahead = me + 2
    behind = me - 2
    tp_x = tp // 2
    tp_c = lax.rem(tp, 2)
    tp_mate = tp_x * 2 + (1 - tp_c)
    has_next = outer < outer_n - 1
    has_prev = outer > 0

    w_copies = (
        pltpu.make_async_copy(wd_ref, weights.at[pl.ds(0, diff_rows)], w_sem.at[0]),
        pltpu.make_async_copy(
            wl_ref, weights.at[pl.ds(diff_rows, wl_ref.shape[0])], w_sem.at[1]
        ),
    )
    for copy in w_copies:
        copy.start()

    barrier = pltpu.get_barrier_semaphore()

    def greet(where):
        pl.semaphore_signal(barrier, inc=1, device_id=where, device_id_type=MESH)

    greet({"sp": mate})
    greet({"tp": tp_mate})
    for step in range(1, half):
        greet({"tp": lax.rem(tp_x + step, half) * 2 + tp_c})

    @pl.when(has_next)
    def _():
        greet({"sp": ahead})

    @pl.when(has_prev)
    def _():
        greet({"sp": behind})

    pl.semaphore_wait(
        barrier, 1 + half + has_next.astype(jnp.int32) + has_prev.astype(jnp.int32)
    )

    def remote(src, dst, send, recv, where):
        return pltpu.make_async_remote_copy(
            src_ref=src,
            dst_ref=dst,
            send_sem=send,
            recv_sem=recv,
            device_id=where,
            device_id_type=MESH,
        )

    def z_k(s, src):
        return remote(src, zk.at[s + 1], zk_send.at[s], zk_recv.at[s + 1], {"sp": ahead})

    def z_v(s, src):
        return remote(src, zv.at[s + 1], zv_send.at[s], zv_recv.at[s + 1], {"sp": ahead})

    def y_k(s, src):
        return remote(src, yk.at[s], yk_send.at[s], yk_recv.at[s], {"sp": mate})

    def y_v(s, src):
        return remote(src, yv.at[s], yv_send.at[s], yv_recv.at[s], {"sp": mate})

    @pl.when(has_next)
    def _():
        z_k(0, k_ref).start()

    @pl.when(inner == 0)
    def _():
        y_k(0, k_ref).start()

    @pl.when(has_next)
    def _():
        z_v(0, v_ref).start()

    @pl.when(inner == 0)
    def _():
        y_v(0, v_ref).start()

    for g in range(kv_here):
        for m in range(2):
            for j in range(group):
                col = ((g * group + j) * 2 + m) * HEAD_DIM
                qs[g, m, pl.ds(j * tok, tok), :] = q_ref[:, pl.ds(col, HEAD_DIM)]

    rate = math.log2(math.e) / math.sqrt(HEAD_DIM)
    stacked = group * tok

    def attend(key_ref, value_ref, first, ready=None):
        kept = {}
        for g in range(kv_here):
            for m in range(2):
                key = key_ref[:, pl.ds((g * 2 + m) * HEAD_DIM, HEAD_DIM)]
                scores = dot(qs[g, m], key, NT)
                if first:
                    at_row = lax.rem(lax.broadcasted_iota(jnp.int32, (stacked, tok), 0), tok)
                    at_col = lax.broadcasted_iota(jnp.int32, (stacked, tok), 1)
                    scores = jnp.where(at_row >= at_col, scores, neg_large)
                best = jnp.max(scores, axis=-1, keepdims=True)
                if not first:
                    old = top[g, m]
                    best = jnp.maximum(old, best)
                expo = jnp.exp2((scores - best) * rate)
                add = jnp.sum(expo, axis=-1, keepdims=True)
                top[g, m] = best
                shrink = None
                if first:
                    total[g, m] = add
                else:
                    shrink = jnp.exp2((old - best) * rate)
                    total[g, m] = total[g, m] * shrink + add
                kept[g, m] = (expo.astype(BF16), shrink)
        if ready is not None:
            ready()
        for g in range(kv_here):
            value = value_ref[:, pl.ds(g * VAL_DIM, VAL_DIM)]
            for m in range(2):
                expo, shrink = kept[g, m]
                grown = dot(expo, value, NN)
                numer[g, m] = grown if first else numer[g, m] * shrink + grown

    attend(k_ref, v_ref, True)

    def pass_key(s):
        remote(zk.at[s], zk.at[s], zk_send.at[s], zk_recv.at[s], {"sp": mate}).wait_recv()

        @pl.when(has_next)
        def _():
            z_k(s, zk.at[s]).start()

        y_k(s, zk.at[s]).start()

    def pass_value(s):
        remote(zv.at[s], zv.at[s], zv_send.at[s], zv_recv.at[s], {"sp": mate}).wait_recv()

        @pl.when(has_next)
        def _():
            z_v(s, zv.at[s]).start()

        y_v(s, zv.at[s]).start()

    length = math.gcd(tok, BLOCK)
    low = lax.broadcasted_iota(jnp.int32, (length, length), 0) >= lax.broadcasted_iota(
        jnp.int32, (length, length), 1
    )
    tri = low.astype(F32)
    for h in range(lin_heads):
        kc = pl.ds(h * KEY_DIM, KEY_DIM)
        vc = pl.ds(h * VAL_DIM, VAL_DIM)
        state = None
        passed = jnp.zeros((1, KEY_DIM), F32)
        for b in range(tok // length):
            r = pl.ds(b * length, length)
            pre = pre_ref[r, kc]
            log_decay = (jnp.minimum(pre, 0.0) - jnp.log1p(jnp.exp(-jnp.abs(pre)))) / gate_temp
            cumulative = dot(tri, log_decay, NN, highest)
            last = cumulative[length - 1 :, :]
            query = lq_ref[r, kc].astype(F32) * (KEY_DIM**-0.5) * jnp.exp(cumulative)
            key = lk_ref[r, kc].astype(F32)
            value = lv_ref[r, vc].astype(F32)
            inside = dot(query, key * jnp.exp(-cumulative), NT, highest)
            inside = jnp.where(low, inside, 0.0)
            rows = dot(inside, value, NN, highest)
            fresh = dot(value, key * jnp.exp(last - cumulative), TN, highest)
            if state is not None:
                rows = rows + dot(query, state, NT, highest)
                fresh = fresh + jnp.exp(last) * state
            rows_ref[r, vc] = rows
            reach[r, kc] = query * jnp.exp(passed)
            state = fresh
            passed = passed + last
            if h == lin_heads - 1 and b == (tok // length) // 2 - 1:

                @pl.when(has_prev)
                def _():
                    pass_key(1)

        own_state[h, pl.ds(0, VAL_DIM), :] = state
        own_state[h, pl.ds(VAL_DIM, 8), :] = jnp.broadcast_to(passed, (8, KEY_DIM))
        msg[h, pl.ds(0, VAL_DIM), :] = state.astype(BF16)
        high = passed.astype(BF16).astype(F32)
        pick = lax.broadcasted_iota(jnp.int32, (16, KEY_DIM), 0) < 8
        msg[h, pl.ds(VAL_DIM, 16), :] = jnp.where(pick, high, passed - high).astype(BF16)

    s_copy = remote(msg, got, s_send, s_recv, {"sp": mate})
    s_copy.start()

    @pl.when(has_prev)
    def _():
        pass_value(1)


    def from_mate(t):
        y_k(t, yk.at[t]).wait_recv()
        attend(yk.at[t], yv.at[t], False, lambda: y_v(t, yv.at[t]).wait_recv())

    def hop(s, carry):
        @pl.when(s > 1)
        def _():
            pass_key(s)
            pass_value(s)

        attend(zk.at[s], zv.at[s], False)

        @pl.when((s > 1) | (inner == 1))
        def _():
            from_mate(s - 1)

        return carry

    lax.fori_loop(1, outer + 1, hop, 0)

    s_copy.wait_recv()
    c_copy = remote(chain_out, chain_in, c_send, c_recv, {"sp": ahead})

    @pl.when(has_prev)
    def _():
        c_copy.wait_recv()

    @pl.when(jnp.logical_not(has_prev))
    def _():
        chain_in[...] = jnp.zeros_like(chain_in)

    for h in range(lin_heads):
        mine = own_state[h, pl.ds(0, VAL_DIM), :]
        mine_decay = own_state[h, pl.ds(VAL_DIM, 8), :][:1]
        theirs = got[h, pl.ds(0, VAL_DIM), :].astype(F32)
        tail = got[h, pl.ds(VAL_DIM, 16), :].astype(F32)
        theirs_decay = tail[:1] + tail[8:9]
        before = chain_in[h].astype(F32)
        to_first = jnp.exp(theirs_decay) * before + theirs
        incoming = jnp.where(inner == 1, to_first, before)
        both = jnp.exp(mine_decay) * to_first + mine
        other = jnp.exp(theirs_decay) * (jnp.exp(mine_decay) * before + mine) + theirs
        chain_out[h] = jnp.where(inner == 1, both, other).astype(BF16)
        own_state[h, pl.ds(0, VAL_DIM), :] = incoming

    @pl.when(has_next)
    def _():
        c_copy.start()

    for h in range(lin_heads):
        kc = pl.ds(h * KEY_DIM, KEY_DIM)
        vc = pl.ds(h * VAL_DIM, VAL_DIM)
        rows = rows_ref[:, vc] + dot(
            reach[:, kc], own_state[h, pl.ds(0, VAL_DIM), :], NT, highest
        )
        act[:, pl.ds(diff_rows + h * VAL_DIM, VAL_DIM)] = head_norm(
            rows, lgain_ref[:, vc]
        ).astype(BF16)

    @pl.when(has_prev | (inner == 1))
    def _():
        from_mate(outer)

    for g in range(kv_here):
        for j in range(group):
            h = g * group + j
            r = pl.ds(j * tok, tok)
            attended = numer[g, 0, r, :] / total[g, 0, r, :] - lam_ref[h] * (
                numer[g, 1, r, :] / total[g, 1, r, :]
            )
            act[:, pl.ds(h * VAL_DIM, VAL_DIM)] = head_norm(attended, dgain_ref[...]).astype(BF16)

    for copy in w_copies:
        copy.wait()

    width = part.shape[-1]
    pieces = part.shape[0]
    rows_each = tok // n_tp

    def pair_copy(j):
        return remote(
            part.at[j, 1 - tp_c], pair_buf.at[j], p_send.at[j], p_recv.at[j], {"tp": tp_mate}
        )

    def cross_copy(j, step):
        to = lax.rem(tp_x + step, half)
        return remote(
            sum_buf.at[j, step - 1],
            cross_buf.at[j, step - 1],
            x_send.at[j, step - 1],
            x_recv.at[j, step - 1],
            {"tp": to * 2 + tp_c},
        )

    def reduce_pair(j):
        pair_copy(j).wait_recv()
        for step in range(1, half):
            to = lax.rem(tp_x + step, half)
            sum_buf[j, step - 1] = (
                part[j, tp_c, to].astype(F32) + pair_buf[j, to].astype(F32)
            ).astype(BF16)
            cross_copy(j, step).start()
        own_sum[j] = part[j, tp_c, tp_x].astype(F32) + pair_buf[j, tp_x].astype(F32)

    def project(j, carry):
        cols = pl.ds(pl.multiple_of(j * width, width), width)
        piece = dot(act[...], weights[:, cols], NN).astype(BF16)
        for a in range(half):
            for c in range(2):
                part[j, c, a] = piece[(a * 2 + c) * rows_each : (a * 2 + c + 1) * rows_each]
        pair_copy(j).start()

        @pl.when(j > 0)
        def _():
            reduce_pair(j - 1)

        return carry

    lax.fori_loop(0, pieces, project, 0)
    reduce_pair(pieces - 1)

    def finish(j, carry):
        cols = pl.ds(pl.multiple_of(j * width, width), width)
        whole = own_sum[j]
        for step in range(1, half):
            cross_copy(j, step).wait_recv()
            whole = whole + cross_buf[j, step - 1].astype(F32)
        out_ref[:, cols] = whole.astype(BF16)
        pair_copy(j).wait_send()
        for step in range(1, half):
            cross_copy(j, step).wait_send()
        return carry

    lax.fori_loop(0, pieces, finish, 0)

    s_copy.wait_send()

    @pl.when(inner == 0)
    def _():
        y_k(0, k_ref).wait_send()
        y_v(0, v_ref).wait_send()

    @pl.when(has_next)
    def _():
        z_k(0, k_ref).wait_send()
        z_v(0, v_ref).wait_send()
        c_copy.wait_send()

    def drain(s, carry):
        y_k(s, zk.at[s]).wait_send()
        y_v(s, zv.at[s]).wait_send()

        @pl.when(has_next)
        def _():
            z_k(s, zk.at[s]).wait_send()
            z_v(s, zv.at[s]).wait_send()

        return carry

    lax.fori_loop(1, outer + 1, drain, 0)


def body(
    n_sp,
    n_tp,
    queries,
    keys,
    values,
    lam,
    diff_gain,
    lin_query,
    lin_key,
    lin_value,
    decay_pre,
    lin_gain,
    w_out_diff,
    w_out_lin,
):
    tok = queries.shape[0]
    kv_here = keys.shape[1] // (2 * HEAD_DIM)
    heads = queries.shape[1] // (2 * HEAD_DIM)
    lin_heads = lin_query.shape[1] // KEY_DIM
    model = w_out_diff.shape[1]
    in_rows = w_out_diff.shape[0] + w_out_lin.shape[0]
    stacked = heads // kv_here * tok
    width = math.gcd(model, PIECE)
    pieces = model // width
    half = n_tp // 2
    outer_n = n_sp // 2
    rows_each = tok // n_tp
    vmem = pl.BlockSpec(memory_space=pltpu.VMEM)
    anywhere = pl.BlockSpec(memory_space=pl.ANY)
    smem = pl.BlockSpec(memory_space=pltpu.SMEM)
    dma = pltpu.SemaphoreType.DMA
    return pl.pallas_call(
        functools.partial(kernel, n_sp, n_tp),
        out_shape=jax.ShapeDtypeStruct((rows_each, model), BF16),
        in_specs=[vmem] * 3 + [smem] + [vmem] * 6 + [anywhere] * 2,
        out_specs=vmem,
        scratch_shapes=[
            pltpu.VMEM((outer_n, *keys.shape), BF16),
            pltpu.VMEM((outer_n, *values.shape), BF16),
            pltpu.VMEM((outer_n, *keys.shape), BF16),
            pltpu.VMEM((outer_n, *values.shape), BF16),
            pltpu.VMEM((kv_here, 2, stacked, HEAD_DIM), BF16),
            pltpu.VMEM((kv_here, 2, stacked, 1), F32),
            pltpu.VMEM((kv_here, 2, stacked, 1), F32),
            pltpu.VMEM((kv_here, 2, stacked, VAL_DIM), F32),
            pltpu.VMEM((lin_heads, VAL_DIM + 16, KEY_DIM), BF16),
            pltpu.VMEM((lin_heads, VAL_DIM + 16, KEY_DIM), BF16),
            pltpu.VMEM((lin_heads, VAL_DIM, KEY_DIM), BF16),
            pltpu.VMEM((lin_heads, VAL_DIM, KEY_DIM), BF16),
            pltpu.VMEM((lin_heads, VAL_DIM + 8, KEY_DIM), F32),
            pltpu.VMEM(lin_query.shape, F32),
            pltpu.VMEM(lin_value.shape, F32),
            pltpu.VMEM((tok, in_rows), BF16),
            pltpu.VMEM((in_rows, model), BF16),
            pltpu.VMEM((pieces, 2, half, rows_each, width), BF16),
            pltpu.VMEM((pieces, half, rows_each, width), BF16),
            pltpu.VMEM((pieces, half - 1, rows_each, width), BF16),
            pltpu.VMEM((pieces, rows_each, width), F32),
            pltpu.VMEM((pieces, half - 1, rows_each, width), BF16),
            dma((2,)),
        ]
        + [dma((outer_n,))] * 8
        + [dma] * 4
        + [dma((pieces,))] * 2
        + [dma((pieces, half - 1))] * 2,
        compiler_params=pltpu.CompilerParams(
            collective_id=0, has_side_effects=True, vmem_limit_bytes=60 * 1024 * 1024
        ),
    )(
        queries,
        keys,
        values,
        lam,
        diff_gain.reshape(1, -1),
        lin_query,
        lin_key,
        lin_value,
        decay_pre,
        lin_gain.reshape(1, -1),
        w_out_diff,
        w_out_lin,
    )


def solution(mesh):
    return jax.shard_map(
        functools.partial(body, mesh.shape["sp"], mesh.shape["tp"]),
        mesh=mesh,
        in_specs=(
            P("sp", "tp"),
            P("sp", "tp"),
            P("sp", "tp"),
            P("tp"),
            P(),
            P("sp", "tp"),
            P("sp", "tp"),
            P("sp", "tp"),
            P("sp", "tp"),
            P("tp"),
            P("tp", None),
            P("tp", None),
        ),
        out_specs=P(("sp", "tp"), None),
        check_vma=False,
    )
```

```python
import functools
import math

import jax
import jax.numpy as jnp
from jax import lax
from jax.experimental import pallas as pl
from jax.experimental.pallas import tpu as pltpu
from jax.sharding import PartitionSpec as P

HEAD_DIM = 128
KEY_DIM = 128
VAL_DIM = 256
BLOCK = 64
PIECE = 256
LAG = 3

norm_eps = 1e-06
gate_temp = 16.0
neg_large = -1e30
highest = lax.Precision.HIGHEST
MESH = pl.DeviceIdType.MESH
F32 = jnp.float32
BF16 = jnp.bfloat16


def dot(a, b, dims, precision=None):
    return lax.dot_general(
        a, b, (dims, ((), ())), precision=precision, preferred_element_type=F32
    )


NN = ((1,), (0,))
NT = ((1,), (1,))
TN = ((0,), (0,))


def head_norm(rows, gain):
    return rows * lax.rsqrt(jnp.mean(rows * rows, axis=-1, keepdims=True) + norm_eps) * gain


def kernel(
    n_sp,
    n_tp,
    q_ref,
    k_ref,
    v_ref,
    lam_ref,
    dgain_ref,
    lq_ref,
    lk_ref,
    lv_ref,
    pre_ref,
    lgain_ref,
    wd_ref,
    wl_ref,
    out_ref,
    zk,
    zv,
    yk,
    yv,
    qs,
    top,
    total,
    numer,
    msg,
    got,
    chain_in,
    chain_out,
    own_state,
    reach,
    rows_ref,
    act,
    weights,
    part,
    pair_buf,
    sum_buf,
    own_sum,
    cross_buf,
    w_sem,
    zk_send,
    zk_recv,
    zv_send,
    zv_recv,
    yk_send,
    yk_recv,
    yv_send,
    yv_recv,
    s_send,
    s_recv,
    c_send,
    c_recv,
    p_send,
    p_recv,
    x_send,
    x_recv,
):
    outer_n = n_sp // 2
    half = n_tp // 2
    tok = q_ref.shape[0]
    kv_here = k_ref.shape[1] // (2 * HEAD_DIM)
    heads = q_ref.shape[1] // (2 * HEAD_DIM)
    group = heads // kv_here
    lin_heads = lq_ref.shape[1] // KEY_DIM
    diff_rows = wd_ref.shape[0]
    me = lax.axis_index("sp")
    tp = lax.axis_index("tp")
    outer = me // 2
    inner = lax.rem(me, 2)
    mate = outer * 2 + (1 - inner)
    ahead = me + 2
    behind = me - 2
    tp_x = tp // 2
    tp_c = lax.rem(tp, 2)
    tp_mate = tp_x * 2 + (1 - tp_c)
    has_next = outer < outer_n - 1
    has_prev = outer > 0

    w_copies = (
        pltpu.make_async_copy(wd_ref, weights.at[pl.ds(0, diff_rows)], w_sem.at[0]),
        pltpu.make_async_copy(
            wl_ref, weights.at[pl.ds(diff_rows, wl_ref.shape[0])], w_sem.at[1]
        ),
    )
    for copy in w_copies:
        copy.start()

    barrier = pltpu.get_barrier_semaphore()

    def greet(where):
        pl.semaphore_signal(barrier, inc=1, device_id=where, device_id_type=MESH)

    greet({"sp": mate})
    greet({"tp": tp_mate})
    for step in range(1, half):
        greet({"tp": lax.rem(tp_x + step, half) * 2 + tp_c})

    @pl.when(has_next)
    def _():
        greet({"sp": ahead})

    @pl.when(has_prev)
    def _():
        greet({"sp": behind})

    pl.semaphore_wait(
        barrier, 1 + half + has_next.astype(jnp.int32) + has_prev.astype(jnp.int32)
    )

    def remote(src, dst, send, recv, where):
        return pltpu.make_async_remote_copy(
            src_ref=src,
            dst_ref=dst,
            send_sem=send,
            recv_sem=recv,
            device_id=where,
            device_id_type=MESH,
        )

    def z_k(s, src):
        return remote(src, zk.at[s + 1], zk_send.at[s], zk_recv.at[s + 1], {"sp": ahead})

    def z_v(s, src):
        return remote(src, zv.at[s + 1], zv_send.at[s], zv_recv.at[s + 1], {"sp": ahead})

    def y_k(s, src):
        return remote(src, yk.at[s], yk_send.at[s], yk_recv.at[s], {"sp": mate})

    def y_v(s, src):
        return remote(src, yv.at[s], yv_send.at[s], yv_recv.at[s], {"sp": mate})

    @pl.when(has_next)
    def _():
        z_k(0, k_ref).start()

    @pl.when(inner == 0)
    def _():
        y_k(0, k_ref).start()

    @pl.when(has_next)
    def _():
        z_v(0, v_ref).start()

    @pl.when(inner == 0)
    def _():
        y_v(0, v_ref).start()

    for g in range(kv_here):
        for m in range(2):
            for j in range(group):
                col = ((g * group + j) * 2 + m) * HEAD_DIM
                qs[g, m, pl.ds(j * tok, tok), :] = q_ref[:, pl.ds(col, HEAD_DIM)]

    rate = math.log2(math.e) / math.sqrt(HEAD_DIM)
    stacked = group * tok

    def attend(key_ref, value_ref, first, ready=None):
        kept = {}
        for g in range(kv_here):
            for m in range(2):
                key = key_ref[:, pl.ds((g * 2 + m) * HEAD_DIM, HEAD_DIM)]
                scores = dot(qs[g, m], key, NT)
                if first:
                    at_row = lax.rem(lax.broadcasted_iota(jnp.int32, (stacked, tok), 0), tok)
                    at_col = lax.broadcasted_iota(jnp.int32, (stacked, tok), 1)
                    scores = jnp.where(at_row >= at_col, scores, neg_large)
                best = jnp.max(scores, axis=-1, keepdims=True)
                if not first:
                    old = top[g, m]
                    best = jnp.maximum(old, best)
                expo = jnp.exp2((scores - best) * rate)
                add = jnp.sum(expo, axis=-1, keepdims=True)
                top[g, m] = best
                shrink = None
                if first:
                    total[g, m] = add
                else:
                    shrink = jnp.exp2((old - best) * rate)
                    total[g, m] = total[g, m] * shrink + add
                kept[g, m] = (expo.astype(BF16), shrink)
        if ready is not None:
            ready()
        for g in range(kv_here):
            value = value_ref[:, pl.ds(g * VAL_DIM, VAL_DIM)]
            for m in range(2):
                expo, shrink = kept[g, m]
                grown = dot(expo, value, NN)
                numer[g, m] = grown if first else numer[g, m] * shrink + grown

    attend(k_ref, v_ref, True)

    def pass_key(s):
        remote(zk.at[s], zk.at[s], zk_send.at[s], zk_recv.at[s], {"sp": mate}).wait_recv()

        @pl.when(has_next)
        def _():
            z_k(s, zk.at[s]).start()

        y_k(s, zk.at[s]).start()

    def pass_value(s):
        remote(zv.at[s], zv.at[s], zv_send.at[s], zv_recv.at[s], {"sp": mate}).wait_recv()

        @pl.when(has_next)
        def _():
            z_v(s, zv.at[s]).start()

        y_v(s, zv.at[s]).start()

    length = math.gcd(tok, BLOCK)
    low = lax.broadcasted_iota(jnp.int32, (length, length), 0) >= lax.broadcasted_iota(
        jnp.int32, (length, length), 1
    )
    tri = low.astype(F32)
    for h in range(lin_heads):
        kc = pl.ds(h * KEY_DIM, KEY_DIM)
        vc = pl.ds(h * VAL_DIM, VAL_DIM)
        state = None
        passed = jnp.zeros((1, KEY_DIM), F32)
        for b in range(tok // length):
            r = pl.ds(b * length, length)
            pre = pre_ref[r, kc]
            log_decay = (jnp.minimum(pre, 0.0) - jnp.log1p(jnp.exp(-jnp.abs(pre)))) / gate_temp
            cumulative = dot(tri, log_decay, NN, highest)
            last = cumulative[length - 1 :, :]
            query = lq_ref[r, kc].astype(F32) * (KEY_DIM**-0.5) * jnp.exp(cumulative)
            key = lk_ref[r, kc].astype(F32)
            value = lv_ref[r, vc].astype(F32)
            inside = dot(query, key * jnp.exp(-cumulative), NT, highest)
            inside = jnp.where(low, inside, 0.0)
            rows = dot(inside, value, NN, highest)
            fresh = dot(value, key * jnp.exp(last - cumulative), TN, highest)
            if state is not None:
                rows = rows + dot(query, state, NT, highest)
                fresh = fresh + jnp.exp(last) * state
            rows_ref[r, vc] = rows
            reach[r, kc] = query * jnp.exp(passed)
            state = fresh
            passed = passed + last
            if h == lin_heads - 1 and b == (tok // length) // 2 - 1:

                @pl.when(has_prev)
                def _():
                    pass_key(1)

        own_state[h, pl.ds(0, VAL_DIM), :] = state
        own_state[h, pl.ds(VAL_DIM, 8), :] = jnp.broadcast_to(passed, (8, KEY_DIM))
        msg[h, pl.ds(0, VAL_DIM), :] = state.astype(BF16)
        high = passed.astype(BF16).astype(F32)
        pick = lax.broadcasted_iota(jnp.int32, (16, KEY_DIM), 0) < 8
        msg[h, pl.ds(VAL_DIM, 16), :] = jnp.where(pick, high, passed - high).astype(BF16)

    s_copy = remote(msg, got, s_send, s_recv, {"sp": mate})
    s_copy.start()

    @pl.when(has_prev)
    def _():
        pass_value(1)


    def from_mate(t):
        y_k(t, yk.at[t]).wait_recv()
        attend(yk.at[t], yv.at[t], False, lambda: y_v(t, yv.at[t]).wait_recv())

    def hop(s, carry):
        @pl.when(s > 1)
        def _():
            pass_key(s)
            pass_value(s)

        attend(zk.at[s], zv.at[s], False)

        @pl.when((s > 1) | (inner == 1))
        def _():
            from_mate(s - 1)

        return carry

    lax.fori_loop(1, outer + 1, hop, 0)

    s_copy.wait_recv()
    c_copy = remote(chain_out, chain_in, c_send, c_recv, {"sp": ahead})

    @pl.when(has_prev)
    def _():
        c_copy.wait_recv()

    @pl.when(jnp.logical_not(has_prev))
    def _():
        chain_in[...] = jnp.zeros_like(chain_in)

    for h in range(lin_heads):
        mine = own_state[h, pl.ds(0, VAL_DIM), :]
        mine_decay = own_state[h, pl.ds(VAL_DIM, 8), :][:1]
        theirs = got[h, pl.ds(0, VAL_DIM), :].astype(F32)
        tail = got[h, pl.ds(VAL_DIM, 16), :].astype(F32)
        theirs_decay = tail[:1] + tail[8:9]
        before = chain_in[h].astype(F32)
        to_first = jnp.exp(theirs_decay) * before + theirs
        incoming = jnp.where(inner == 1, to_first, before)
        both = jnp.exp(mine_decay) * to_first + mine
        other = jnp.exp(theirs_decay) * (jnp.exp(mine_decay) * before + mine) + theirs
        chain_out[h] = jnp.where(inner == 1, both, other).astype(BF16)
        own_state[h, pl.ds(0, VAL_DIM), :] = incoming

    @pl.when(has_next)
    def _():
        c_copy.start()

    for h in range(lin_heads):
        kc = pl.ds(h * KEY_DIM, KEY_DIM)
        vc = pl.ds(h * VAL_DIM, VAL_DIM)
        rows = rows_ref[:, vc] + dot(
            reach[:, kc], own_state[h, pl.ds(0, VAL_DIM), :], NT, highest
        )
        act[:, pl.ds(diff_rows + h * VAL_DIM, VAL_DIM)] = head_norm(
            rows, lgain_ref[:, vc]
        ).astype(BF16)

    @pl.when(has_prev | (inner == 1))
    def _():
        from_mate(outer)

    for g in range(kv_here):
        for j in range(group):
            h = g * group + j
            r = pl.ds(j * tok, tok)
            attended = numer[g, 0, r, :] / total[g, 0, r, :] - lam_ref[h] * (
                numer[g, 1, r, :] / total[g, 1, r, :]
            )
            act[:, pl.ds(h * VAL_DIM, VAL_DIM)] = head_norm(attended, dgain_ref[...]).astype(BF16)

    for copy in w_copies:
        copy.wait()

    width = part.shape[-1]
    pieces = part.shape[0]
    rows_each = tok // n_tp

    def pair_copy(j):
        return remote(
            part.at[j, 1 - tp_c], pair_buf.at[j], p_send.at[j], p_recv.at[j], {"tp": tp_mate}
        )

    def cross_copy(j, step):
        to = lax.rem(tp_x + step, half)
        return remote(
            sum_buf.at[j, step - 1],
            cross_buf.at[j, step - 1],
            x_send.at[j, step - 1],
            x_recv.at[j, step - 1],
            {"tp": to * 2 + tp_c},
        )

    def reduce_pair(j):
        pair_copy(j).wait_recv()
        for step in range(1, half):
            to = lax.rem(tp_x + step, half)
            sum_buf[j, step - 1] = (
                part[j, tp_c, to].astype(F32) + pair_buf[j, to].astype(F32)
            ).astype(BF16)
            cross_copy(j, step).start()
        own_sum[j] = part[j, tp_c, tp_x].astype(F32) + pair_buf[j, tp_x].astype(F32)

    def project(j, carry):
        cols = pl.ds(pl.multiple_of(j * width, width), width)
        piece = dot(act[...], weights[:, cols], NN).astype(BF16)
        for a in range(half):
            for c in range(2):
                part[j, c, a] = piece[(a * 2 + c) * rows_each : (a * 2 + c + 1) * rows_each]
        pair_copy(j).start()

        @pl.when(j >= LAG)
        def _():
            reduce_pair(j - LAG)

        return carry

    lax.fori_loop(0, pieces, project, 0)

    def reduce_rest(j, carry):
        reduce_pair(j)
        return carry

    lax.fori_loop(max(pieces - LAG, 0), pieces, reduce_rest, 0)

    def finish(j, carry):
        cols = pl.ds(pl.multiple_of(j * width, width), width)
        whole = own_sum[j]
        for step in range(1, half):
            cross_copy(j, step).wait_recv()
            whole = whole + cross_buf[j, step - 1].astype(F32)
        out_ref[:, cols] = whole.astype(BF16)
        pair_copy(j).wait_send()
        for step in range(1, half):
            cross_copy(j, step).wait_send()
        return carry

    lax.fori_loop(0, pieces, finish, 0)

    s_copy.wait_send()

    @pl.when(inner == 0)
    def _():
        y_k(0, k_ref).wait_send()
        y_v(0, v_ref).wait_send()

    @pl.when(has_next)
    def _():
        z_k(0, k_ref).wait_send()
        z_v(0, v_ref).wait_send()
        c_copy.wait_send()

    def drain(s, carry):
        y_k(s, zk.at[s]).wait_send()
        y_v(s, zv.at[s]).wait_send()

        @pl.when(has_next)
        def _():
            z_k(s, zk.at[s]).wait_send()
            z_v(s, zv.at[s]).wait_send()

        return carry

    lax.fori_loop(1, outer + 1, drain, 0)


def body(
    n_sp,
    n_tp,
    queries,
    keys,
    values,
    lam,
    diff_gain,
    lin_query,
    lin_key,
    lin_value,
    decay_pre,
    lin_gain,
    w_out_diff,
    w_out_lin,
):
    tok = queries.shape[0]
    kv_here = keys.shape[1] // (2 * HEAD_DIM)
    heads = queries.shape[1] // (2 * HEAD_DIM)
    lin_heads = lin_query.shape[1] // KEY_DIM
    model = w_out_diff.shape[1]
    in_rows = w_out_diff.shape[0] + w_out_lin.shape[0]
    stacked = heads // kv_here * tok
    width = math.gcd(model, PIECE)
    pieces = model // width
    half = n_tp // 2
    outer_n = n_sp // 2
    rows_each = tok // n_tp
    vmem = pl.BlockSpec(memory_space=pltpu.VMEM)
    anywhere = pl.BlockSpec(memory_space=pl.ANY)
    smem = pl.BlockSpec(memory_space=pltpu.SMEM)
    dma = pltpu.SemaphoreType.DMA
    return pl.pallas_call(
        functools.partial(kernel, n_sp, n_tp),
        out_shape=jax.ShapeDtypeStruct((rows_each, model), BF16),
        in_specs=[vmem] * 3 + [smem] + [vmem] * 6 + [anywhere] * 2,
        out_specs=vmem,
        scratch_shapes=[
            pltpu.VMEM((outer_n, *keys.shape), BF16),
            pltpu.VMEM((outer_n, *values.shape), BF16),
            pltpu.VMEM((outer_n, *keys.shape), BF16),
            pltpu.VMEM((outer_n, *values.shape), BF16),
            pltpu.VMEM((kv_here, 2, stacked, HEAD_DIM), BF16),
            pltpu.VMEM((kv_here, 2, stacked, 1), F32),
            pltpu.VMEM((kv_here, 2, stacked, 1), F32),
            pltpu.VMEM((kv_here, 2, stacked, VAL_DIM), F32),
            pltpu.VMEM((lin_heads, VAL_DIM + 16, KEY_DIM), BF16),
            pltpu.VMEM((lin_heads, VAL_DIM + 16, KEY_DIM), BF16),
            pltpu.VMEM((lin_heads, VAL_DIM, KEY_DIM), BF16),
            pltpu.VMEM((lin_heads, VAL_DIM, KEY_DIM), BF16),
            pltpu.VMEM((lin_heads, VAL_DIM + 8, KEY_DIM), F32),
            pltpu.VMEM(lin_query.shape, F32),
            pltpu.VMEM(lin_value.shape, F32),
            pltpu.VMEM((tok, in_rows), BF16),
            pltpu.VMEM((in_rows, model), BF16),
            pltpu.VMEM((pieces, 2, half, rows_each, width), BF16),
            pltpu.VMEM((pieces, half, rows_each, width), BF16),
            pltpu.VMEM((pieces, half - 1, rows_each, width), BF16),
            pltpu.VMEM((pieces, rows_each, width), F32),
            pltpu.VMEM((pieces, half - 1, rows_each, width), BF16),
            dma((2,)),
        ]
        + [dma((outer_n,))] * 8
        + [dma] * 4
        + [dma((pieces,))] * 2
        + [dma((pieces, half - 1))] * 2,
        compiler_params=pltpu.CompilerParams(
            collective_id=0, has_side_effects=True, vmem_limit_bytes=60 * 1024 * 1024
        ),
    )(
        queries,
        keys,
        values,
        lam,
        diff_gain.reshape(1, -1),
        lin_query,
        lin_key,
        lin_value,
        decay_pre,
        lin_gain.reshape(1, -1),
        w_out_diff,
        w_out_lin,
    )


def solution(mesh):
    return jax.shard_map(
        functools.partial(body, mesh.shape["sp"], mesh.shape["tp"]),
        mesh=mesh,
        in_specs=(
            P("sp", "tp"),
            P("sp", "tp"),
            P("sp", "tp"),
            P("tp"),
            P(),
            P("sp", "tp"),
            P("sp", "tp"),
            P("sp", "tp"),
            P("sp", "tp"),
            P("tp"),
            P("tp", None),
            P("tp", None),
        ),
        out_specs=P(("sp", "tp"), None),
        check_vma=False,
    )
```
